32 devices in a mesh: ep: 8 (over z, core), tp: 4 (over y, x).
Axes of the slice: x: 2, y: 2, z: 4, core: 2. Of those that a mesh axis runs over, the one named last changes fastest.
Arguments:
- first_batch_queries: bfloat16 [2048, 1024], P('ep', 'tp'), may hold values from -6 to 6
- first_batch_keys: bfloat16 [2048, 1024], P('ep', 'tp'), may hold values from -6 to 6
- first_batch_values: bfloat16 [2048, 2048], P('ep', 'tp'), may hold values from -6 to 6
- output_gate_preactivation: bfloat16 [2048, 2048], P('ep', 'tp'), may hold values from -6 to 6
- decay_preactivation: bfloat16 [2048, 1024], P('ep', 'tp'), may hold values from -6 to 6
- channel_decay_bias: float32 [1024], P('tp')
- added_log_decay: float32 [16, 2048], P('tp', 'ep'), may hold values from -0.7 to 0
- head_norm_gain: float32 [2048], P('tp'), may hold values from 0.1 to 1.9
- attention_output_weight: bfloat16 [2048, 2048], P(None, 'tp'), may hold values from -0.125 to 0.125
- second_batch_rows: bfloat16 [768, 2048], P('ep'), may hold values from -6 to 6
- expert_norm_gain: float32 [2048], replicated, may hold values from 0.1 to 1.9
- routed_expert_index: int32 [768, 4], P('ep'), may hold values from 0 to 7, all different within a row; in each aligned block of 96 rows (0 to 95, 96 to 191, ...) at most 72 rows name the same one
- router_chosen_scores: float32 [768, 4], P('ep'), may hold values from 0.1 to 1
- expert_gate_weight: bfloat16 [8, 2048, 4096], P('ep', None, 'tp'), may hold values from -0.125 to 0.125
- expert_up_weight: bfloat16 [8, 2048, 4096], P('ep', None, 'tp'), may hold values from -0.125 to 0.125
- expert_down_weight: bfloat16 [8, 4096, 2048], P('ep', None, 'tp'), may hold values from -0.09375 to 0.09375
- shared_gate_weight: bfloat16 [2048, 1024], P(None, 'tp'), may hold values from -0.125 to 0.125
- shared_up_weight: bfloat16 [2048, 1024], P(None, 'tp'), may hold values from -0.125 to 0.125
- shared_down_weight: bfloat16 [1024, 2048], P(None, 'tp'), may hold values from -0.1875 to 0.1875
Outputs:
- token_mixed: bfloat16 [2048, 2048], P('ep', 'tp')
- channel_mixed: bfloat16 [768, 2048], P('ep', 'tp')
The draws below stay inside these ranges and needn't reach their ends.
Inputs may be any that keep to these rules, and one draw needn't show every extreme that they name: `routed_expert_index`: in each aligned block of 96 rows (the rows of one index of ep) no expert is named by more than 72 rows, a bound that some block reaches; a row names 4 different experts.
All inputs are finite; a program needn't handle non-finite values.
Results may differ from the reference program's by a relative error of at most 0.018.
Values may be sent and summed in bfloat16 or wider, within the bound.
A program may use at most 64 MiB of HBM per device.

```python
import math
from functools import partial
import jax
import jax.numpy as jnp
import numpy as np
from jax import lax

D = 2048
ATTENTION_HEADS = 16
DK = 64
DV = 128
BLOCK = 64
FFE = 4096
FFS = 1024
TOPK = 4
TOK_A = 256
TOK_B = 96
FIRST_TOKENS = 2048
TOKENS_B = 768
EXPERTS = 8
CAP = 72


def draw_channel_decay_bias(key, part):
    key_kind, key_slow, key_fast = jax.random.split(jax.random.fold_in(key, 11), 3)
    share = 0.5
    slow_head = jax.random.uniform(key_kind, (ATTENTION_HEADS, 1), jnp.float32) < share
    slow_level = math.log(0.34 * FIRST_TOKENS) + jax.random.uniform(key_slow, (ATTENTION_HEADS, DK), jnp.float32, -0.5, 0.5)
    fast_level = jax.random.uniform(key_fast, (ATTENTION_HEADS, DK), jnp.float32, -1.0, 1.5)
    return jnp.where(slow_head, slow_level, fast_level).reshape(ATTENTION_HEADS * DK).astype(jnp.float32)


def draw_added_log_decay(key, part):
    key_rate, key_locations, key_dimension = jax.random.split(jax.random.fold_in(key, 23), 3)
    devices = FIRST_TOKENS // TOK_A
    device_rates = jnp.exp(jax.random.uniform(key_rate, (devices,), jnp.float32, math.log(0.1), math.log(1.0))) / FIRST_TOKENS
    baseline_log_decay = -jnp.repeat(device_rates, TOK_A)
    position_index = jnp.arange(FIRST_TOKENS, dtype=jnp.int32)
    half_length = FIRST_TOKENS // 2
    halves_start = jnp.array([0, half_length], dtype=jnp.int32)
    spike_positions = jax.random.randint(key_locations, (ATTENTION_HEADS, 2), 0, half_length) + halves_start[None, :]
    spike_magnitude = jnp.log(jax.random.uniform(key_dimension, (ATTENTION_HEADS, 2), jnp.float32, 0.5, 0.8))
    decay_spikes = jnp.sum(jnp.where(position_index[None, None, :] == spike_positions[:, :, None], spike_magnitude[:, :, None], 0.0), axis=1)
    return (baseline_log_decay[None, :] + decay_spikes).astype(jnp.float32)


def block_scale(rng, shape, cuts, low, top_value):
    gain, own = 1.0, jax.random.fold_in(rng, 6)
    for dim, parts in cuts:
        steps = jnp.exp(jax.random.uniform(jax.random.fold_in(own, dim), (parts,), jnp.float32, low / len(cuts), top_value / len(cuts)))
        gain = gain * jnp.repeat(steps, shape[dim] // parts).reshape([-1 if axis == dim else 1 for axis in range(len(shape))])
    return gain


def shared_out(key, own, number, rows, amount, top, bound, slope):
    sequence = jax.random.permutation(key, amount)
    heavy_load, ordinary = load_shares(amount, rows * top, bound, slope, True), load_shares(amount, rows * top, bound, slope, False)
    places = jnp.arange(amount)

    def named(lengths, rotation):
        used = int((lengths > 0).sum())
        fixed = max(1, used // 4)
        shifted = fixed + (places - fixed + rotation * (used - fixed)) % max(1, amount - fixed)
        return jnp.zeros((amount,), jnp.int32).at[sequence[jnp.where(places < fixed, places, shifted)]].set(jnp.asarray(lengths, jnp.int32))

    lengths = jnp.where(number % 4 == 0, named(heavy_load, number // 4), named(ordinary, number - number // 4 - 1))
    mixed = jax.random.permutation(jax.random.fold_in(own, 3), amount)
    source_of, receiver = mixed[0:amount // 2 * 2:2], mixed[1:amount // 2 * 2:2]
    room = jnp.minimum(lengths[source_of] - 1, bound - lengths[receiver]) // 2
    room = jnp.where((source_of == sequence[0]) | (receiver == sequence[0]) | (lengths[receiver] == 0), 0, jnp.maximum(room, 0))
    shifted = jax.random.randint(jax.random.fold_in(own, 4), (amount // 2,), 0, 1 << 20) % (room + 1)
    lengths = lengths.at[source_of].add(-shifted).at[receiver].add(shifted)
    labels = jnp.searchsorted(jnp.cumsum(lengths), jnp.arange(rows * top), side="right").astype(jnp.int32)
    table = labels.reshape(top, rows).T
    table = table[jax.random.permutation(jax.random.fold_in(own, 1), rows)]
    rotation = jax.random.randint(jax.random.fold_in(own, 2), (rows, 1), 0, top)
    return jnp.take_along_axis(table, (jnp.arange(top)[None, :] + rotation) % top, axis=1)


def load_shares(count, total, reach, skew, full):
    weights = [(1 << 20) // math.isqrt(grade ** skew) + 1 for grade in range(1, count + 1)]
    largest = reach if full else min(reach, max(-(-total // count), total * weights[0] // sum(weights)))
    least = 1 if total - largest >= count - 1 else 0
    counts, surplus = [largest] + [least] * (count - 1), total - largest - least * (count - 1)
    while surplus > 0:
        candidates = [i for i in range(1, count) if counts[i] < largest] or [i for i in range(1, count) if counts[i] < reach]
        whole, budget = sum([weights[i] for i in candidates]), surplus
        for i in candidates:
            extra = min(reach - counts[i], max(1, budget * weights[i] // whole), surplus)
            counts[i] = counts[i] + extra
            surplus = surplus - extra
    return np.array(counts)


def normal_values(key, dims, deviation, limit, pieces=(), kind=jnp.bfloat16):
    values = deviation * jax.random.normal(key, dims, jnp.float32)
    if pieces:
        values = values * block_scale(key, dims, pieces, -0.22, 0.18)
    return jnp.clip(values, -limit, limit).astype(kind)


def setup_inputs(seed: int = 0) -> dict:
    streams_of = jax.random.split(jax.random.key(seed), 20)
    first_batch_queries = normal_values(streams_of[0], (FIRST_TOKENS, ATTENTION_HEADS * DK), 1.0, 6.0, ((0, 8), (1, 4)))
    first_batch_keys = normal_values(streams_of[1], (FIRST_TOKENS, ATTENTION_HEADS * DK), 1.0, 6.0, ((0, 8), (1, 4)))
    first_batch_values = normal_values(streams_of[2], (FIRST_TOKENS, ATTENTION_HEADS * DV), 1.0, 6.0, ((0, 8), (1, 4)))
    output_gate_preactivation = normal_values(streams_of[3], (FIRST_TOKENS, ATTENTION_HEADS * DV), 1.0, 6.0, ((0, 8), (1, 4)))
    decay_preactivation = normal_values(streams_of[4], (FIRST_TOKENS, ATTENTION_HEADS * DK), 1.0, 6.0, ((0, 8), (1, 4)))
    channel_decay_bias = draw_channel_decay_bias(jax.random.fold_in(streams_of[19], 71), 0)
    added_log_decay = draw_added_log_decay(jax.random.fold_in(streams_of[19], 71), 0)
    head_norm_gain = jnp.clip(1.0 + 0.18 * jax.random.normal(streams_of[7], (ATTENTION_HEADS * DV,), jnp.float32), 0.1, 1.9)
    attention_output_weight = normal_values(streams_of[8], (ATTENTION_HEADS * DV, D), (ATTENTION_HEADS * DV) ** -0.5, 0.125, ((1, 4),))
    second_batch_rows = normal_values(streams_of[9], (TOKENS_B, D), 1.0, 6.0, ((0, 8),))
    expert_norm_gain = jnp.clip(1.0 + 0.18 * jax.random.normal(streams_of[10], (D,), jnp.float32), 0.1, 1.9)
    routed_expert_index_keys = jax.random.split(jax.random.fold_in(streams_of[11], 1), TOKENS_B // TOK_B)
    routed_expert_index_turns = jax.random.permutation(jax.random.fold_in(streams_of[11], 3), TOKENS_B // TOK_B)
    routed_expert_index = jax.vmap(lambda own, number: shared_out(jax.random.fold_in(streams_of[11], 2), own, number, TOK_B, EXPERTS, TOPK, CAP, 1))(routed_expert_index_keys, routed_expert_index_turns).reshape((TOKENS_B, TOPK))
    router_chosen_scores = jnp.clip(jnp.exp(math.log(1.0) - 2.3025851 * jax.random.uniform(streams_of[12], (TOKENS_B, TOPK), jnp.float32) ** block_scale(streams_of[12], (TOKENS_B, TOPK), ((0, 8),), -0.2, 0.2)), 0.1, 1.0)
    expert_gate_weight = normal_values(streams_of[13], (EXPERTS, D, FFE), D ** -0.5, 0.125, ((0, 8), (2, 4)))
    expert_up_weight = normal_values(streams_of[14], (EXPERTS, D, FFE), D ** -0.5, 0.125, ((0, 8), (2, 4)))
    expert_down_weight = normal_values(streams_of[15], (EXPERTS, FFE, D), FFE ** -0.5, 0.09375, ((0, 8), (2, 4)))
    shared_gate_weight = normal_values(streams_of[16], (D, FFS), D ** -0.5, 0.125, ((1, 4),))
    shared_up_weight = normal_values(streams_of[17], (D, FFS), D ** -0.5, 0.125, ((1, 4),))
    shared_down_weight = normal_values(streams_of[18], (FFS, D), FFS ** -0.5, 0.1875, ((1, 4),))
    return {"first_batch_queries": first_batch_queries, "first_batch_keys": first_batch_keys, "first_batch_values": first_batch_values, "output_gate_preactivation": output_gate_preactivation, "decay_preactivation": decay_preactivation, "channel_decay_bias": channel_decay_bias, "added_log_decay": added_log_decay, "head_norm_gain": head_norm_gain, "attention_output_weight": attention_output_weight, "second_batch_rows": second_batch_rows, "expert_norm_gain": expert_norm_gain, "routed_expert_index": routed_expert_index, "router_chosen_scores": router_chosen_scores, "expert_gate_weight": expert_gate_weight, "expert_up_weight": expert_up_weight, "expert_down_weight": expert_down_weight, "shared_gate_weight": shared_gate_weight, "shared_up_weight": shared_up_weight, "shared_down_weight": shared_down_weight}


epsilon = 1e-06
temper = 16.0
routed_scale = 2.5
largest_value = lax.Precision.HIGHEST

def head_norm(tensor, gain_rows):
    mean_square = lax.optimization_barrier(jnp.mean(tensor * tensor, axis=-1, keepdims=True))
    return tensor * lax.rsqrt(mean_square + epsilon) * gain_rows

def log_decay_values(decay_preactivation, channel_decay_bias, added_log_decay):
    number_of_heads = added_log_decay.shape[0]
    row_count = decay_preactivation.shape[0]
    logits = decay_preactivation.astype(jnp.float32) + channel_decay_bias[None, :]
    baseline_log_decay = (jax.nn.log_sigmoid(logits) / temper).reshape(row_count, number_of_heads, -1)
    return baseline_log_decay + jnp.transpose(added_log_decay)[:, :, None]

def gated_linear(queries, keys_all, values, decay_factors):
    row_count, number_of_heads, key_channel_width = queries.shape
    value_width = values.shape[-1]
    block_count = row_count // BLOCK

    def split_into_blocks(tensor):
        return tensor.reshape(block_count, BLOCK, number_of_heads, tensor.shape[-1]).transpose(0, 2, 1, 3)
    lower_mask = jnp.tril(jnp.ones((BLOCK, BLOCK), bool))

    def advance(carry_state, inputs):
        query_block, block_of_keys, block_of_values, decay_block = inputs
        running_state = jnp.cumsum(decay_block, axis=1)
        query_decayed = query_block * jnp.exp(running_state)
        key_raised = block_of_keys * jnp.exp(-running_state)
        attention_scores = jnp.einsum('hqd,hkd->hqk', query_decayed, key_raised, precision=largest_value)
        attention_scores = jnp.where(lower_mask, attention_scores, 0.0)
        within_block = jnp.einsum('gnx,gxy->gny', attention_scores, block_of_values, precision=largest_value)
        carried = jnp.einsum('hqd,hdv->hqv', query_decayed, carry_state, precision=largest_value)
        block_number_total = running_state[:, -1:, :]
        state_update = jnp.einsum('ien,ieg->ing', block_of_keys * jnp.exp(block_number_total - running_state), block_of_values, precision=largest_value)
        new_state = jnp.exp(block_number_total[:, 0, :])[..., None] * carry_state + state_update
        return (new_state, within_block + carried)
    start_state = jnp.zeros((number_of_heads, key_channel_width, value_width), jnp.float32)
    _, outputs = lax.scan(advance, start_state, (split_into_blocks(queries), split_into_blocks(keys_all), split_into_blocks(values), split_into_blocks(decay_factors)))
    return outputs.transpose(0, 2, 1, 3).reshape(row_count, number_of_heads, value_width)

def expert_slots(route_rows, experts, capacity):
    flat_ids = route_rows.reshape(-1)
    targets = jnp.arange(experts, dtype=jnp.int32)
    onehot = (flat_ids[:, None] == targets[None, :]).astype(jnp.int32)
    earlier = jnp.cumsum(onehot, axis=0) - onehot
    return (flat_ids * capacity + lax.optimization_barrier(jnp.sum(earlier * onehot, axis=1))).astype(jnp.int32)

def slot_owner(slot_ids, slot_count, top_count):
    matches = slot_ids[None, :] == jnp.arange(slot_count, dtype=jnp.int32)[:, None]
    token_ids = jnp.arange(slot_ids.shape[0], dtype=jnp.int32) // top_count
    return (lax.optimization_barrier(jnp.sum(jnp.where(matches, token_ids[None, :] + 1, 0), axis=1)) - 1).astype(jnp.int32)

def reference(first_batch_queries, first_batch_keys, first_batch_values, output_gate_preactivation, decay_preactivation, channel_decay_bias, added_log_decay, head_norm_gain, attention_output_weight, second_batch_rows, expert_norm_gain, routed_expert_index, router_chosen_scores, expert_gate_weight, expert_up_weight, expert_down_weight, shared_gate_weight, shared_up_weight, shared_down_weight):
    decay_factors = log_decay_values(decay_preactivation, channel_decay_bias, added_log_decay)
    queries = first_batch_queries.astype(jnp.float32).reshape(FIRST_TOKENS, ATTENTION_HEADS, DK)
    keys_all = first_batch_keys.astype(jnp.float32).reshape(FIRST_TOKENS, ATTENTION_HEADS, DK)
    values = first_batch_values.astype(jnp.float32).reshape(FIRST_TOKENS, ATTENTION_HEADS, DV)
    head_values = gated_linear(queries, keys_all, values, decay_factors)
    gate_rows = jax.nn.silu(output_gate_preactivation.astype(jnp.float32)).reshape(FIRST_TOKENS, ATTENTION_HEADS, DV)
    mixed_heads = head_norm(head_values, head_norm_gain.reshape(ATTENTION_HEADS, DV)) * gate_rows
    mixed_heads = mixed_heads.reshape(FIRST_TOKENS, ATTENTION_HEADS * DV).astype(jnp.bfloat16)
    token_mixed = jnp.dot(mixed_heads, attention_output_weight, preferred_element_type=jnp.float32).astype(jnp.bfloat16)
    features = second_batch_rows.astype(jnp.float32)
    normed = features * lax.rsqrt(lax.optimization_barrier(jnp.mean(features * features, axis=1, keepdims=True)) + epsilon)
    normed = (normed * expert_norm_gain[None, :]).astype(jnp.bfloat16)
    sources = TOKENS_B // TOK_B
    slot_count = EXPERTS * CAP
    block_routes = routed_expert_index.reshape(sources, TOK_B, TOPK)
    slot_ids = jax.vmap(partial(expert_slots, experts=EXPERTS, capacity=CAP))(block_routes)
    owners = jax.vmap(partial(slot_owner, slot_count=slot_count, top_count=TOPK))(slot_ids)
    offsets = (jnp.arange(sources, dtype=jnp.int32) * TOK_B)[:, None]
    global_owner = jnp.where(owners >= 0, owners + offsets, -1)
    per_expert = global_owner.reshape(sources, EXPERTS, CAP).transpose(1, 0, 2).reshape(EXPERTS, sources * CAP)

    def run_expert(inputs):
        owner_rows, gate_weight, up_weight, down_weight = inputs
        picked_rows = jnp.take(normed, jnp.maximum(owner_rows, 0), axis=0)
        rows_in = jnp.where((owner_rows >= 0)[:, None], picked_rows, jnp.zeros((), jnp.bfloat16))
        gate_value = jnp.dot(rows_in, gate_weight, preferred_element_type=jnp.float32)
        up_value = jnp.dot(rows_in, up_weight, preferred_element_type=jnp.float32)
        hidden = (jax.nn.silu(gate_value) * up_value).astype(jnp.bfloat16)
        return jnp.dot(hidden, down_weight, preferred_element_type=jnp.float32).astype(jnp.bfloat16)
    results = lax.map(run_expert, (per_expert, expert_gate_weight, expert_up_weight, expert_down_weight))
    expert_ids = block_routes.reshape(sources, -1)
    source_ids = jnp.arange(sources, dtype=jnp.int32)[:, None]
    flat_index = expert_ids * (sources * CAP) + source_ids * CAP + (slot_ids - expert_ids * CAP)
    picked = jnp.take(results.reshape(-1, D), flat_index.reshape(-1).astype(jnp.int32), axis=0)
    picked = picked.astype(jnp.float32).reshape(TOKENS_B, TOPK, D)
    weights = routed_scale * router_chosen_scores / lax.optimization_barrier(jnp.sum(router_chosen_scores, axis=1, keepdims=True))
    shared_gate_value = jnp.dot(normed, shared_gate_weight, preferred_element_type=jnp.float32)
    shared_up_value = jnp.dot(normed, shared_up_weight, preferred_element_type=jnp.float32)
    shared_hidden = (jax.nn.silu(shared_gate_value) * shared_up_value).astype(jnp.bfloat16)
    shared_total = jnp.dot(shared_hidden, shared_down_weight, preferred_element_type=jnp.float32)
    channel_mixed = (lax.optimization_barrier(jnp.sum(weights[:, :, None] * picked, axis=1)) + shared_total).astype(jnp.bfloat16)
    return (token_mixed, channel_mixed)
```

```python
import functools

import jax
import jax.numpy as jnp
from jax import lax
from jax.experimental import pallas as pl
from jax.experimental.pallas import tpu as pltpu
from jax.sharding import PartitionSpec as P

BLOCK = 64
LANES = 128

epsilon = 1e-06
temper = 16.0
routed_scale = 2.5
exact = lax.Precision.HIGHEST
bf16 = jnp.bfloat16
f32 = jnp.float32


NT = (((1,), (1,)), ((), ()))
TN = (((0,), (0,)), ((), ()))


def shifted(value, axis, step, flip=0):
    size = lax.axis_size(axis)
    pairs = [(i, ((i + 2 * step) % size) ^ flip) for i in range(size)]
    return lax.ppermute(value, axis, pairs)


def swapped(value, axis, bit):
    size = lax.axis_size(axis)
    return lax.ppermute(value, axis, [(i, i ^ bit) for i in range(size)])


def gathered(value):
    if lax.axis_size("tp") != 4:
        return lax.all_gather(value, "tp", axis=1, tiled=True)
    half = value.shape[0] // 2 // 8 * 8
    one = swapped(value, "tp", 1)
    two = swapped(value, "tp", 2)
    upper = swapped(one[:half], "tp", 2)
    lower = swapped(two[half:], "tp", 1)
    return (value, one, two, (upper, lower))


def weight_blocks(weight):
    parts = lax.axis_size("tp")
    if parts != 4:
        return weight
    depth = weight.shape[0] // parts
    here = lax.axis_index("tp")
    return [
        lax.dynamic_slice_in_dim(weight, (here ^ k) * depth, depth, 0) for k in range(parts)
    ]


def gathered_dot(blocks, weights):
    def mul(a, b):
        return jnp.dot(a, b, preferred_element_type=f32)

    if lax.axis_size("tp") != 4:
        return mul(blocks, weights)
    own, one, two, (upper, lower) = blocks
    first = mul(own, weights[0]) + mul(one, weights[1]) + mul(two, weights[2])
    last = mul(jnp.concatenate([upper, lower], axis=0), weights[3])
    return first + last


def block_kernel(
    heads, q_ref, k_ref, v_ref, decay_ref, within_ref, lead_ref, state_ref, total_ref
):
    rows, channels = q_ref.shape
    width = channels // heads
    value_width = v_ref.shape[1] // heads
    row_id = lax.broadcasted_iota(jnp.int32, (BLOCK, BLOCK), 0)
    col_id = lax.broadcasted_iota(jnp.int32, (BLOCK, BLOCK), 1)
    lower = row_id >= col_id
    ones = lower.astype(f32)
    state = jnp.zeros((value_width, channels), f32)
    passed = jnp.zeros((1, channels), f32)
    for n in range(rows // BLOCK):
        span = pl.ds(n * BLOCK, BLOCK)
        running = jnp.dot(ones, decay_ref[span, :], precision=exact, preferred_element_type=f32)
        total = running[BLOCK - 1 :, :]
        q = q_ref[span, :].astype(f32) * jnp.exp(running)
        k = k_ref[span, :].astype(f32)
        raised = (k * jnp.exp(-running)).astype(bf16)
        update = (k * jnp.exp(total - running)).astype(bf16)
        lead_ref[span, :] = (q * jnp.exp(passed)).astype(bf16)
        q = q.astype(bf16)
        held = state.astype(bf16)
        added = []
        for h in range(heads):
            lanes = slice(h * width, (h + 1) * width)
            v = v_ref[span, h * value_width : (h + 1) * value_width]
            scores = lax.dot_general(q[:, lanes], raised[:, lanes], NT, preferred_element_type=f32)
            scores = jnp.where(lower, scores, 0.0).astype(bf16)
            within = jnp.dot(scores, v, preferred_element_type=f32)
            if n > 0:
                within += lax.dot_general(
                    q[:, lanes], held[:, lanes], NT, preferred_element_type=f32
                )
            within_ref[span, h * value_width : (h + 1) * value_width] = within
            added.append(
                lax.dot_general(v, update[:, lanes], TN, preferred_element_type=f32)
            )
        state = state * jnp.exp(total) + jnp.concatenate(added, axis=1)
        passed = passed + total
    state_ref[...] = state
    total_ref[...] = jnp.exp(passed)


def finish_kernel(heads, within_ref, lead_ref, incoming_ref, gain_ref, gate_ref, out_ref):
    width = lead_ref.shape[1] // heads
    value_width = within_ref.shape[1] // heads
    for h in range(heads):
        lanes = slice(h * width, (h + 1) * width)
        columns = slice(h * value_width, (h + 1) * value_width)
        value = within_ref[:, columns] + lax.dot_general(
            lead_ref[:, lanes], incoming_ref[:, lanes], NT, preferred_element_type=f32
        )
        mean_square = jnp.mean(value * value, axis=-1, keepdims=True)
        gate = gate_ref[:, columns].astype(f32)
        gate = gate / (1.0 + jnp.exp(-gate))
        out_ref[:, columns] = (
            value * lax.rsqrt(mean_square + epsilon) * gain_ref[:, columns] * gate
        ).astype(bf16)


def decay_rows(decay_preactivation, channel_decay_bias, added_log_decay):
    width = decay_preactivation.shape[1] // added_log_decay.shape[0]
    logits = decay_preactivation.astype(f32) + channel_decay_bias[None, :]
    spread = jnp.repeat(jnp.transpose(added_log_decay), width, axis=1)
    return jax.nn.log_sigmoid(logits) / temper + spread


def entering(state, decay):
    size = lax.axis_size("ep")
    rows = state.shape[0]
    tail = 16

    def hop(state, decay, distance):
        packed = jnp.concatenate(
            [state.astype(bf16), jnp.broadcast_to(decay.astype(bf16), (tail, decay.shape[1]))]
        )
        came = lax.ppermute(packed, "ep", [(i, i + distance) for i in range(size - distance)])
        return came[:rows].astype(f32), came[rows : rows + 1].astype(f32)

    state, decay = hop(state, decay, 1)
    distance = 1
    while distance < size:
        earlier, earlier_decay = hop(state, decay, distance)
        state = decay * earlier + state
        decay = decay * earlier_decay
        distance *= 2
    return state.astype(bf16)


def attention_local(q, k, v, decay, heads):
    rows, channels = q.shape
    value_width = v.shape[1] // heads
    return pl.pallas_call(
        functools.partial(block_kernel, heads),
        out_shape=(
            jax.ShapeDtypeStruct(v.shape, f32),
            jax.ShapeDtypeStruct(q.shape, bf16),
            jax.ShapeDtypeStruct((value_width, channels), f32),
            jax.ShapeDtypeStruct((1, channels), f32),
        ),
        cost_estimate=pl.CostEstimate(
            flops=6 * rows * BLOCK * v.shape[1], bytes_accessed=4 * v.size, transcendentals=4 * q.size
        ),
        name="blocks",
    )(q, k, v, decay)


def attention_finish(within, lead, incoming, gain, gate, heads):
    return pl.pallas_call(
        functools.partial(finish_kernel, heads),
        out_shape=jax.ShapeDtypeStruct(within.shape, bf16),
        cost_estimate=pl.CostEstimate(
            flops=8 * within.size, bytes_accessed=8 * within.size, transcendentals=within.size
        ),
        name="finish",
    )(within, lead, incoming, gain, gate)


def ring_blocks(own):
    chips = lax.axis_size("ep") // 2
    blocks = {0: own}
    ahead = behind = own
    for step in range(1, (chips - 1) // 2 + 1):
        ahead = shifted(ahead, "ep", 1)
        behind = shifted(behind, "ep", -1)
        blocks[step] = ahead
        blocks[chips - step] = behind
    if chips % 2 == 0:
        half = own.shape[0] // 2 // 8 * 8
        upper = shifted(ahead[:half], "ep", 1)
        lower = shifted(behind[half:], "ep", -1)
        blocks[chips // 2] = jnp.concatenate([upper, lower], axis=0)
    return blocks


def expert_rows(block, expert, width, top_count, capacity):
    tokens = block.shape[0]
    named = block[:, width : width + top_count]
    match = jnp.any(named == expert.astype(bf16), axis=1)
    before = (
        lax.broadcasted_iota(jnp.int32, (tokens, tokens), 0)
        < lax.broadcasted_iota(jnp.int32, (tokens, tokens), 1)
    )
    rank = jnp.sum(jnp.where(before & match[:, None], 1, 0), axis=0)
    rank = jnp.where(match, rank, -1)
    pick = (lax.broadcasted_iota(jnp.int32, (capacity, tokens), 0) == rank[None, :]).astype(bf16)
    return jnp.dot(pick, block[:, :width], preferred_element_type=f32).astype(bf16)


def local(
    first_batch_queries,
    first_batch_keys,
    first_batch_values,
    output_gate_preactivation,
    decay_preactivation,
    channel_decay_bias,
    added_log_decay,
    head_norm_gain,
    attention_output_weight,
    second_batch_rows,
    expert_norm_gain,
    routed_expert_index,
    router_chosen_scores,
    expert_gate_weight,
    expert_up_weight,
    expert_down_weight,
    shared_gate_weight,
    shared_up_weight,
    shared_down_weight,
):
    experts = lax.axis_size("ep")
    chips = experts // 2
    here = lax.axis_index("ep")
    heads = added_log_decay.shape[0]
    tokens, top_count = routed_expert_index.shape
    capacity = tokens * top_count * 3 // (2 * experts)
    width = second_batch_rows.shape[1]

    features = second_batch_rows.astype(f32)
    normed = features * lax.rsqrt(jnp.mean(features * features, axis=1, keepdims=True) + epsilon)
    normed = (normed * expert_norm_gain[None, :]).astype(bf16)
    named = jnp.pad(routed_expert_index.astype(bf16), ((0, 0), (0, LANES - top_count)))
    mine = ring_blocks(jnp.concatenate([normed, named], axis=1))

    gate_weight, up_weight = expert_gate_weight[0], expert_up_weight[0]
    down_blocks = weight_blocks(expert_down_weight[0])
    mix_blocks = weight_blocks(attention_output_weight)
    shared_blocks = weight_blocks(shared_down_weight)

    order = sorted(range(chips), key=lambda d: (min(d, chips - d), d))
    groups = {}
    for d in order:
        groups.setdefault(min(d, chips - d), []).append(d)

    hidden = {}
    for key, members in groups.items():
        rows = []
        for d in members:
            for flip in range(2):
                block = mine[d] if flip == 0 else swapped(mine[d], "ep", 1)
                rows.append(expert_rows(block, here, width, top_count, capacity))
        rows = jnp.concatenate(rows, axis=0)
        gate_value = jnp.dot(rows, gate_weight, preferred_element_type=f32)
        up_value = jnp.dot(rows, up_weight, preferred_element_type=f32)
        hidden[key] = gathered((jax.nn.silu(gate_value) * up_value).astype(bf16))

    decay = decay_rows(decay_preactivation, channel_decay_bias, added_log_decay)
    within, lead, state, total = attention_local(
        first_batch_queries, first_batch_keys, first_batch_values, decay, heads
    )
    incoming = entering(state, total)
    mixed_heads = attention_finish(
        within, lead, incoming, head_norm_gain[None, :], output_gate_preactivation, heads
    )

    shared_gate_value = jnp.dot(normed, shared_gate_weight, preferred_element_type=f32)
    shared_up_value = jnp.dot(normed, shared_up_weight, preferred_element_type=f32)
    shared_hidden = (jax.nn.silu(shared_gate_value) * shared_up_value).astype(bf16)
    shared_total = gathered_dot(gathered(shared_hidden), shared_blocks)
    token_mixed = gathered_dot(gathered(mixed_heads), mix_blocks).astype(bf16)

    weights = (
        routed_scale * router_chosen_scores / jnp.sum(router_chosen_scores, axis=1, keepdims=True)
    )
    earlier = (
        lax.broadcasted_iota(jnp.int32, (tokens, tokens), 1)
        < lax.broadcasted_iota(jnp.int32, (tokens, tokens), 0)
    )
    slots = lax.broadcasted_iota(jnp.int32, (tokens, capacity), 1)
    summed = shared_total
    for key, members in groups.items():
        output = gathered_dot(hidden[key], down_blocks).astype(bf16)
        returned, picks = [], []
        for number, d in enumerate(members):
            for flip in range(2):
                start = (2 * number + flip) * capacity
                piece = output[start : start + capacity]
                if d == 0:
                    piece = piece if flip == 0 else swapped(piece, "ep", 1)
                else:
                    piece = shifted(piece, "ep", -d, flip)
                returned.append(piece)
                source = ((here // 2 + d) % chips * 2 + here % 2) ^ flip
                match = routed_expert_index == source
                weight = jnp.sum(jnp.where(match, weights, 0.0), axis=1)
                chosen = jnp.any(match, axis=1)
                rank = jnp.sum(jnp.where(earlier & chosen[None, :], 1, 0), axis=1)
                rank = jnp.where(chosen, rank, -1)
                picks.append(jnp.where(slots == rank[:, None], weight[:, None], 0.0))
        summed = summed + jnp.dot(
            jnp.concatenate(picks, axis=1),
            jnp.concatenate(returned, axis=0).astype(f32),
            precision=exact,
            preferred_element_type=f32,
        )
    return (token_mixed, summed.astype(bf16))


def solution(mesh):
    placed = (
        P("ep", "tp"),
        P("ep", "tp"),
        P("ep", "tp"),
        P("ep", "tp"),
        P("ep", "tp"),
        P("tp"),
        P("tp", "ep"),
        P("tp"),
        P(None, "tp"),
        P("ep", None),
        P(),
        P("ep", None),
        P("ep", None),
        P("ep", None, "tp"),
        P("ep", None, "tp"),
        P("ep", None, "tp"),
        P(None, "tp"),
        P(None, "tp"),
        P(None, "tp"),
    )
    return jax.shard_map(
        local, mesh=mesh, in_specs=placed, out_specs=(P("ep", "tp"), P("ep", "tp")), check_vma=False
    )
```

```python
import functools

import jax
import jax.numpy as jnp
from jax import lax
from jax.experimental import pallas as pl
from jax.experimental.pallas import tpu as pltpu
from jax.sharding import PartitionSpec as P

BLOCK = 64
LANES = 128

epsilon = 1e-06
temper = 16.0
routed_scale = 2.5
exact = lax.Precision.HIGHEST
bf16 = jnp.bfloat16
f32 = jnp.float32


NT = (((1,), (1,)), ((), ()))
TN = (((0,), (0,)), ((), ()))


def shifted(value, axis, step, flip=0):
    size = lax.axis_size(axis)
    pairs = [(i, ((i + 2 * step) % size) ^ flip) for i in range(size)]
    return lax.ppermute(value, axis, pairs)


def swapped(value, axis, bit):
    size = lax.axis_size(axis)
    return lax.ppermute(value, axis, [(i, i ^ bit) for i in range(size)])


def gathered(value):
    if lax.axis_size("tp") != 4:
        return lax.all_gather(value, "tp", axis=1, tiled=True)
    half = value.shape[0] // 2 // 8 * 8
    one = swapped(value, "tp", 1)
    two = swapped(value, "tp", 2)
    upper = swapped(one[:half], "tp", 2)
    lower = swapped(two[half:], "tp", 1)
    return (value, one, two, (upper, lower))


def weight_blocks(weight):
    parts = lax.axis_size("tp")
    if parts != 4:
        return weight
    depth = weight.shape[0] // parts
    here = lax.axis_index("tp")
    return [
        lax.dynamic_slice_in_dim(weight, (here ^ k) * depth, depth, 0) for k in range(parts)
    ]


def gathered_dot(blocks, weights):
    def mul(a, b):
        return jnp.dot(a, b, preferred_element_type=f32)

    if lax.axis_size("tp") != 4:
        return mul(blocks, weights)
    own, one, two, (upper, lower) = blocks
    first = mul(own, weights[0]) + mul(one, weights[1]) + mul(two, weights[2])
    last = mul(jnp.concatenate([upper, lower], axis=0), weights[3])
    return first + last


def block_kernel(
    heads, q_ref, k_ref, v_ref, decay_ref, within_ref, lead_ref, state_ref, total_ref
):
    rows, channels = q_ref.shape
    width = channels // heads
    value_width = v_ref.shape[1] // heads
    row_id = lax.broadcasted_iota(jnp.int32, (BLOCK, BLOCK), 0)
    col_id = lax.broadcasted_iota(jnp.int32, (BLOCK, BLOCK), 1)
    lower = row_id >= col_id
    ones = lower.astype(f32)
    state = jnp.zeros((value_width, channels), f32)
    passed = jnp.zeros((1, channels), f32)
    for n in range(rows // BLOCK):
        span = pl.ds(n * BLOCK, BLOCK)
        running = jnp.dot(ones, decay_ref[span, :], precision=exact, preferred_element_type=f32)
        total = running[BLOCK - 1 :, :]
        q = q_ref[span, :].astype(f32) * jnp.exp(running)
        k = k_ref[span, :].astype(f32)
        raised = (k * jnp.exp(-running)).astype(bf16)
        update = (k * jnp.exp(total - running)).astype(bf16)
        lead_ref[span, :] = (q * jnp.exp(passed)).astype(bf16)
        q = q.astype(bf16)
        held = state.astype(bf16)
        added = []
        for h in range(heads):
            lanes = slice(h * width, (h + 1) * width)
            v = v_ref[span, h * value_width : (h + 1) * value_width]
            scores = lax.dot_general(q[:, lanes], raised[:, lanes], NT, preferred_element_type=f32)
            scores = jnp.where(lower, scores, 0.0).astype(bf16)
            within = jnp.dot(scores, v, preferred_element_type=f32)
            if n > 0:
                within += lax.dot_general(
                    q[:, lanes], held[:, lanes], NT, preferred_element_type=f32
                )
            within_ref[span, h * value_width : (h + 1) * value_width] = within
            added.append(
                lax.dot_general(v, update[:, lanes], TN, preferred_element_type=f32)
            )
        state = state * jnp.exp(total) + jnp.concatenate(added, axis=1)
        passed = passed + total
    state_ref[...] = state
    total_ref[...] = jnp.exp(passed)


def finish_kernel(heads, within_ref, lead_ref, incoming_ref, gain_ref, gate_ref, out_ref):
    width = lead_ref.shape[1] // heads
    value_width = within_ref.shape[1] // heads
    for h in range(heads):
        lanes = slice(h * width, (h + 1) * width)
        columns = slice(h * value_width, (h + 1) * value_width)
        value = within_ref[:, columns] + lax.dot_general(
            lead_ref[:, lanes], incoming_ref[:, lanes], NT, preferred_element_type=f32
        )
        mean_square = jnp.mean(value * value, axis=-1, keepdims=True)
        gate = gate_ref[:, columns].astype(f32)
        gate = gate / (1.0 + jnp.exp(-gate))
        out_ref[:, columns] = (
            value * lax.rsqrt(mean_square + epsilon) * gain_ref[:, columns] * gate
        ).astype(bf16)


def decay_rows(decay_preactivation, channel_decay_bias, added_log_decay):
    width = decay_preactivation.shape[1] // added_log_decay.shape[0]
    logits = decay_preactivation.astype(f32) + channel_decay_bias[None, :]
    spread = jnp.repeat(jnp.transpose(added_log_decay), width, axis=1)
    return jax.nn.log_sigmoid(logits) / temper + spread


def entering(state, decay):
    size = lax.axis_size("ep")
    rows = state.shape[0]
    tail = 16

    def hop(state, decay, distance):
        packed = jnp.concatenate(
            [state.astype(bf16), jnp.broadcast_to(decay.astype(bf16), (tail, decay.shape[1]))]
        )
        came = lax.ppermute(packed, "ep", [(i, i + distance) for i in range(size - distance)])
        return came[:rows].astype(f32), came[rows : rows + 1].astype(f32)

    state, decay = hop(state, decay, 1)
    distance = 1
    while distance < size:
        earlier, earlier_decay = hop(state, decay, distance)
        state = decay * earlier + state
        decay = decay * earlier_decay
        distance *= 2
    return state.astype(bf16)


def attention_local(q, k, v, decay, heads):
    rows, channels = q.shape
    value_width = v.shape[1] // heads
    return pl.pallas_call(
        functools.partial(block_kernel, heads),
        out_shape=(
            jax.ShapeDtypeStruct(v.shape, f32),
            jax.ShapeDtypeStruct(q.shape, bf16),
            jax.ShapeDtypeStruct((value_width, channels), f32),
            jax.ShapeDtypeStruct((1, channels), f32),
        ),
        cost_estimate=pl.CostEstimate(
            flops=6 * rows * BLOCK * v.shape[1], bytes_accessed=4 * v.size, transcendentals=4 * q.size
        ),
        name="blocks",
    )(q, k, v, decay)


def attention_finish(within, lead, incoming, gain, gate, heads):
    return pl.pallas_call(
        functools.partial(finish_kernel, heads),
        out_shape=jax.ShapeDtypeStruct(within.shape, bf16),
        cost_estimate=pl.CostEstimate(
            flops=8 * within.size, bytes_accessed=8 * within.size, transcendentals=within.size
        ),
        name="finish",
    )(within, lead, incoming, gain, gate)


def ring_blocks(own):
    chips = lax.axis_size("ep") // 2
    blocks = {0: own}
    ahead = behind = own
    for step in range(1, (chips - 1) // 2 + 1):
        ahead = shifted(ahead, "ep", 1)
        behind = shifted(behind, "ep", -1)
        blocks[step] = ahead
        blocks[chips - step] = behind
    if chips % 2 == 0:
        half = own.shape[0] // 2 // 8 * 8
        upper = shifted(ahead[:half], "ep", 1)
        lower = shifted(behind[half:], "ep", -1)
        blocks[chips // 2] = jnp.concatenate([upper, lower], axis=0)
    return blocks


def expert_rows(block, expert, width, top_count, capacity):
    tokens = block.shape[0]
    named = block[:, width : width + top_count]
    match = jnp.any(named == expert.astype(bf16), axis=1)
    before = (
        lax.broadcasted_iota(jnp.int32, (tokens, tokens), 0)
        < lax.broadcasted_iota(jnp.int32, (tokens, tokens), 1)
    )
    rank = jnp.sum(jnp.where(before & match[:, None], 1, 0), axis=0)
    rank = jnp.where(match, rank, -1)
    pick = (lax.broadcasted_iota(jnp.int32, (capacity, tokens), 0) == rank[None, :]).astype(bf16)
    return jnp.dot(pick, block[:, :width], preferred_element_type=f32).astype(bf16)


def local(
    first_batch_queries,
    first_batch_keys,
    first_batch_values,
    output_gate_preactivation,
    decay_preactivation,
    channel_decay_bias,
    added_log_decay,
    head_norm_gain,
    attention_output_weight,
    second_batch_rows,
    expert_norm_gain,
    routed_expert_index,
    router_chosen_scores,
    expert_gate_weight,
    expert_up_weight,
    expert_down_weight,
    shared_gate_weight,
    shared_up_weight,
    shared_down_weight,
):
    experts = lax.axis_size("ep")
    chips = experts // 2
    here = lax.axis_index("ep")
    heads = added_log_decay.shape[0]
    tokens, top_count = routed_expert_index.shape
    capacity = tokens * top_count * 3 // (2 * experts)
    width = second_batch_rows.shape[1]

    features = second_batch_rows.astype(f32)
    normed = features * lax.rsqrt(jnp.mean(features * features, axis=1, keepdims=True) + epsilon)
    normed = (normed * expert_norm_gain[None, :]).astype(bf16)
    named = jnp.pad(routed_expert_index.astype(bf16), ((0, 0), (0, LANES - top_count)))
    mine = ring_blocks(jnp.concatenate([normed, named], axis=1))

    gate_weight, up_weight = expert_gate_weight[0], expert_up_weight[0]
    down_blocks = weight_blocks(expert_down_weight[0])
    mix_blocks = weight_blocks(attention_output_weight)
    shared_blocks = weight_blocks(shared_down_weight)

    order = sorted(range(chips), key=lambda d: (min(d, chips - d), d))
    groups = {}
    for d in order:
        groups.setdefault(min(d, chips - d), []).append(d)

    decay = decay_rows(decay_preactivation, channel_decay_bias, added_log_decay)
    hidden = {}
    for key, members in groups.items():
        rows = []
        for d in members:
            for flip in range(2):
                block = mine[d] if flip == 0 else swapped(mine[d], "ep", 1)
                rows.append(expert_rows(block, here, width, top_count, capacity))
        rows = jnp.concatenate(rows, axis=0)
        gate_value = jnp.dot(rows, gate_weight, preferred_element_type=f32)
        up_value = jnp.dot(rows, up_weight, preferred_element_type=f32)
        made = (jax.nn.silu(gate_value) * up_value).astype(bf16)
        if key == 0:
            made, decay = lax.optimization_barrier((made, decay))
        elif key == 1:
            made, output_gate_preactivation = lax.optimization_barrier(
                (made, output_gate_preactivation)
            )
        if key == chips // 2:
            made, normed, routed_expert_index = lax.optimization_barrier(
                (made, normed, routed_expert_index)
            )
        hidden[key] = gathered(made)

    within, lead, state, total = attention_local(
        first_batch_queries, first_batch_keys, first_batch_values, decay, heads
    )
    incoming = entering(state, total)
    mixed_heads = attention_finish(
        within, lead, incoming, head_norm_gain[None, :], output_gate_preactivation, heads
    )

    shared_gate_value = jnp.dot(normed, shared_gate_weight, preferred_element_type=f32)
    shared_up_value = jnp.dot(normed, shared_up_weight, preferred_element_type=f32)
    shared_hidden = (jax.nn.silu(shared_gate_value) * shared_up_value).astype(bf16)
    shared_total = gathered_dot(gathered(shared_hidden), shared_blocks)
    token_mixed = gathered_dot(gathered(mixed_heads), mix_blocks).astype(bf16)

    weights = (
        routed_scale * router_chosen_scores / jnp.sum(router_chosen_scores, axis=1, keepdims=True)
    )
    earlier = (
        lax.broadcasted_iota(jnp.int32, (tokens, tokens), 1)
        < lax.broadcasted_iota(jnp.int32, (tokens, tokens), 0)
    )
    slots = lax.broadcasted_iota(jnp.int32, (tokens, capacity), 1)
    summed = shared_total
    for key, members in groups.items():
        output = gathered_dot(hidden[key], down_blocks).astype(bf16)
        returned, picks = [], []
        for number, d in enumerate(members):
            for flip in range(2):
                start = (2 * number + flip) * capacity
                piece = output[start : start + capacity]
                if d == 0:
                    piece = piece if flip == 0 else swapped(piece, "ep", 1)
                else:
                    piece = shifted(piece, "ep", -d, flip)
                returned.append(piece)
                source = ((here // 2 + d) % chips * 2 + here % 2) ^ flip
                match = routed_expert_index == source
                weight = jnp.sum(jnp.where(match, weights, 0.0), axis=1)
                chosen = jnp.any(match, axis=1)
                rank = jnp.sum(jnp.where(earlier & chosen[None, :], 1, 0), axis=1)
                rank = jnp.where(chosen, rank, -1)
                picks.append(jnp.where(slots == rank[:, None], weight[:, None], 0.0))
        summed = summed + jnp.dot(
            jnp.concatenate(picks, axis=1),
            jnp.concatenate(returned, axis=0).astype(f32),
            precision=exact,
            preferred_element_type=f32,
        )
    return (token_mixed, summed.astype(bf16))


def solution(mesh):
    placed = (
        P("ep", "tp"),
        P("ep", "tp"),
        P("ep", "tp"),
        P("ep", "tp"),
        P("ep", "tp"),
        P("tp"),
        P("tp", "ep"),
        P("tp"),
        P(None, "tp"),
        P("ep", None),
        P(),
        P("ep", None),
        P("ep", None),
        P("ep", None, "tp"),
        P("ep", None, "tp"),
        P("ep", None, "tp"),
        P(None, "tp"),
        P(None, "tp"),
        P(None, "tp"),
    )
    return jax.shard_map(
        local, mesh=mesh, in_specs=placed, out_specs=(P("ep", "tp"), P("ep", "tp")), check_vma=False
    )
```
